32 devices in a mesh: ep: 4 (over y, x), tp: 8 (over z, core).
Axes of the slice: x: 2, y: 2, z: 4, core: 2. Of those that a mesh axis runs over, the one named last changes fastest.
Arguments:
- tokens: bfloat16 [1024, 4096], P('ep'), may hold values from -6 to 6
- cotangent: bfloat16 [1024, 4096], P('ep'), may hold values from -6 to 6
- routing: int32 [1024, 2], P('ep'), may hold values from 0 to 3, all different within a row; in each aligned block of 256 rows (0 to 255, 256 to 511, ...) at most 160 rows name the same one
- group_gate: float32 [1024], P('ep'), may hold values from 0.2 to 1
- inner_gate: float32 [1024, 2], P('ep'), may hold values from 0.1 to 0.9
- w_gate: bfloat16 [4, 4096, 2048], P('ep', None, 'tp'), may hold values from -0.09375 to 0.09375
- w_up: bfloat16 [4, 4096, 2048], P('ep', None, 'tp'), may hold values from -0.09375 to 0.09375
- w_down: bfloat16 [4, 2048, 4096], P('ep', 'tp'), may hold values from -0.125 to 0.125
Outputs:
- token_grad: bfloat16 [1024, 4096], P('ep', 'tp')
- group_grad: float32 [1024], P('ep')
- inner_grad: float32 [1024, 2], P('ep')
- gate_weight_grad: bfloat16 [4, 4096, 2048], P('ep', None, 'tp')
- up_weight_grad: bfloat16 [4, 4096, 2048], P('ep', None, 'tp')
- down_weight_grad: bfloat16 [4, 2048, 4096], P('ep', 'tp')
The draws below stay inside these ranges and needn't reach their ends.
Inputs may be any that keep to these rules, and one draw needn't show every extreme that they name: `routing`: each row names 2 different experts. Among the rows of one device (aligned blocks of 256 rows) no expert is named more than 160 times, and in every draw some expert is named exactly 160 times in some block.
All inputs are finite; a program needn't handle non-finite values.
Results may differ from the reference program's by a relative error of at most 0.02.
Values may be sent and summed in bfloat16 or wider, within the bound.
A program may use at most 128 MiB of HBM per device.

```python
import math
import jax
import jax.numpy as jnp
import numpy as np
from jax import lax

D = 4096
FF = 2048
TOP = 2
TOK_DEV = 256
EXPERTS = 4
CAP = 160
TOKENS = 1024
N_EP = 4
N_TP = 8


def block_levels(rng, dims, split, least, high):
    factor_of, own = 1.0, jax.random.fold_in(rng, 6)
    for dim, blocks in split:
        draws = jnp.exp(jax.random.uniform(jax.random.fold_in(own, dim), (blocks,), jnp.float32, least / len(split), high / len(split)))
        factor_of = factor_of * jnp.repeat(draws, dims[dim] // blocks).reshape([-1 if axis == dim else 1 for axis in range(len(dims))])
    return factor_of


def deal_out(stream_key, own, number, rows, number_of, top, bound, lean):
    order = jax.random.permutation(stream_key, number_of)
    crowded, usual = load_shares(number_of, rows * top, bound, lean, True), load_shares(number_of, rows * top, bound, lean, False)
    places = jnp.arange(number_of)

    def named(tallies, turn):
        used = int((tallies > 0).sum())
        fixed = max(1, used // 4)
        passed = fixed + (places - fixed + turn * (used - fixed)) % max(1, number_of - fixed)
        return jnp.zeros((number_of,), jnp.int32).at[order[jnp.where(places < fixed, places, passed)]].set(jnp.asarray(tallies, jnp.int32))

    tallies = jnp.where(number % 4 == 0, named(crowded, number // 4), named(usual, number - number // 4 - 1))
    mixed = jax.random.permutation(jax.random.fold_in(own, 3), number_of)
    donor, taker = mixed[0:number_of // 2 * 2:2], mixed[1:number_of // 2 * 2:2]
    margin = jnp.minimum(tallies[donor] - 1, bound - tallies[taker]) // 2
    margin = jnp.where((donor == order[0]) | (taker == order[0]) | (tallies[taker] == 0), 0, jnp.maximum(margin, 0))
    passed = jax.random.randint(jax.random.fold_in(own, 4), (number_of // 2,), 0, 1 << 20) % (margin + 1)
    tallies = tallies.at[donor].add(-passed).at[taker].add(passed)
    members = jnp.searchsorted(jnp.cumsum(tallies), jnp.arange(rows * top), side="right").astype(jnp.int32)
    grid = members.reshape(top, rows).T
    grid = grid[jax.random.permutation(jax.random.fold_in(own, 1), rows)]
    turn = jax.random.randint(jax.random.fold_in(own, 2), (rows, 1), 0, top)
    return jnp.take_along_axis(grid, (jnp.arange(top)[None, :] + turn) % top, axis=1)


def load_shares(amount, total, bound, skew, full):
    portions = [(1 << 20) // math.isqrt(standing ** skew) + 1 for standing in range(1, amount + 1)]
    largest = bound if full else min(bound, max(-(-total // amount), total * portions[0] // sum(portions)))
    least = 1 if total - largest >= amount - 1 else 0
    given, rest = [largest] + [least] * (amount - 1), total - largest - least * (amount - 1)
    while rest > 0:
        movable = [i for i in range(1, amount) if given[i] < largest] or [i for i in range(1, amount) if given[i] < bound]
        mass, budget = sum([portions[i] for i in movable]), rest
        for i in movable:
            more = min(bound - given[i], max(1, budget * portions[i] // mass), rest)
            given[i] = given[i] + more
            rest = rest - more
    return np.array(given)


def centred(own_key, shape, deviation, limit, split=(), kind=jnp.bfloat16):
    drawn = deviation * jax.random.normal(own_key, shape, jnp.float32)
    if split:
        drawn = drawn * block_levels(own_key, shape, split, -0.22, 0.18)
    return jnp.clip(drawn, -limit, limit).astype(kind)


def setup_inputs(seed: int = 0) -> dict:
    seeds = jax.random.split(jax.random.key(seed), 9)
    tokens = centred(seeds[0], (TOKENS, D), 1.0, 6.0, ((0, 4),))
    cotangent = centred(seeds[1], (TOKENS, D), 1.0, 6.0, ((0, 4),))
    routing_keys = jax.random.split(jax.random.fold_in(seeds[2], 1), TOKENS // TOK_DEV)
    routing_turns = jax.random.permutation(jax.random.fold_in(seeds[2], 3), TOKENS // TOK_DEV)
    routing = jax.vmap(lambda own, number: deal_out(jax.random.fold_in(seeds[2], 2), own, number, TOK_DEV, EXPERTS, TOP, CAP, 2))(routing_keys, routing_turns).reshape((TOKENS, TOP))
    group_gate = jnp.clip(0.2 + 0.8 * jax.random.uniform(seeds[3], (TOKENS,), jnp.float32) ** block_levels(seeds[3], (TOKENS,), ((0, 4),), -0.2, 0.2), 0.2, 1.0)
    inner_gate = jnp.clip(0.1 + 0.79999997 * jax.random.uniform(seeds[4], (TOKENS, TOP), jnp.float32) ** block_levels(seeds[4], (TOKENS, TOP), ((0, 4),), -0.2, 0.2), 0.1, 0.9)
    w_gate = centred(seeds[5], (EXPERTS, D, FF), D ** -0.5, 0.09375, ((0, 4), (2, 8)))
    w_up = centred(seeds[6], (EXPERTS, D, FF), D ** -0.5, 0.09375, ((0, 4), (2, 8)))
    w_down = centred(seeds[7], (EXPERTS, FF, D), FF ** -0.5, 0.125, ((0, 4), (1, 8)))
    return dict(tokens=tokens, cotangent=cotangent, routing=routing, group_gate=group_gate, inner_gate=inner_gate, w_gate=w_gate, w_up=w_up, w_down=w_down)


def expert_backward(packed):
    rows_in, cot_rows, row_weight, gate_weight, up_weight, down_weight = packed
    gate_pre = jnp.dot(rows_in, gate_weight, preferred_element_type=jnp.float32)
    up_pre = jnp.dot(rows_in, up_weight, preferred_element_type=jnp.float32)
    sigmoid_gate = jax.nn.sigmoid(gate_pre)
    silu_gate = gate_pre * sigmoid_gate
    hidden = (silu_gate * up_pre).astype(jnp.bfloat16)
    scaled_cot = (row_weight[:, None] * cot_rows.astype(jnp.float32)).astype(jnp.bfloat16)
    down_grad = jnp.dot(hidden.T, scaled_cot, preferred_element_type=jnp.float32).astype(jnp.bfloat16)
    grad_hidden = jnp.dot(cot_rows, down_weight.T, preferred_element_type=jnp.float32)
    scores = jnp.sum(grad_hidden * hidden.astype(jnp.float32), axis=1)
    weighted = row_weight[:, None] * grad_hidden
    grad_gate_in = (weighted * up_pre * sigmoid_gate * (1.0 + gate_pre * (1.0 - sigmoid_gate))).astype(jnp.bfloat16)
    grad_up_in = (weighted * silu_gate).astype(jnp.bfloat16)
    gate_grad = jnp.dot(rows_in.T, grad_gate_in, preferred_element_type=jnp.float32).astype(jnp.bfloat16)
    upper_grad = jnp.dot(rows_in.T, grad_up_in, preferred_element_type=jnp.float32).astype(jnp.bfloat16)
    row_count = rows_in.shape[0]
    model_width = rows_in.shape[1]
    block_units = FF // N_TP
    gate_blocks = grad_gate_in.astype(jnp.float32).reshape(row_count, N_TP, block_units)
    up_blocks = grad_up_in.astype(jnp.float32).reshape(row_count, N_TP, block_units)
    gate_w_blocks = gate_weight.astype(jnp.float32).reshape(model_width, N_TP, block_units)
    up_w_blocks = up_weight.astype(jnp.float32).reshape(model_width, N_TP, block_units)
    partial_rows = (jnp.einsum('rnf,dnf->nrd', gate_blocks, gate_w_blocks, precision=lax.Precision.HIGHEST)
                    + jnp.einsum('rnf,dnf->nrd', up_blocks, up_w_blocks, precision=lax.Precision.HIGHEST))
    rounded_parts = partial_rows.astype(jnp.bfloat16).astype(jnp.float32)
    row_grad = jnp.sum(rounded_parts, axis=0).astype(jnp.bfloat16)
    return gate_grad, upper_grad, down_grad, row_grad, scores


def reference(tokens, cotangent, routing, group_gate, inner_gate, w_gate, w_up, w_down):
    token_count, model_width = tokens.shape
    slots_expert = N_EP * CAP
    total_slots = EXPERTS * slots_expert
    flat_route = routing.reshape(N_EP, TOK_DEV * TOP)
    one_hot = (flat_route[:, :, None] == jnp.arange(EXPERTS, dtype=jnp.int32)[None, None, :]).astype(jnp.int32)
    within = jnp.sum(one_hot * (jnp.cumsum(one_hot, axis=1) - 1), axis=2)
    source = jnp.arange(N_EP, dtype=jnp.int32)[:, None]
    slot_of = (flat_route * slots_expert + source * CAP + within).reshape(-1).astype(jnp.int32)
    token_of = jnp.arange(token_count * TOP, dtype=jnp.int32) // TOP
    combine = (group_gate[:, None] * inner_gate).reshape(-1)
    rows_in = jnp.zeros((total_slots, model_width), jnp.bfloat16).at[slot_of].set(tokens[token_of])
    cot_rows = jnp.zeros((total_slots, model_width), jnp.bfloat16).at[slot_of].set(cotangent[token_of])
    row_weight = jnp.zeros((total_slots,), jnp.float32).at[slot_of].set(combine)
    results = lax.map(expert_backward, (rows_in.reshape(EXPERTS, slots_expert, model_width),
                                        cot_rows.reshape(EXPERTS, slots_expert, model_width),
                                        row_weight.reshape(EXPERTS, slots_expert), w_gate, w_up, w_down))
    gate_grad, upper_grad, down_grad, row_grad, scores = results
    picked = row_grad.reshape(total_slots, model_width)[slot_of].astype(jnp.float32)
    token_grad = jnp.sum(picked.reshape(token_count, TOP, model_width), axis=1).astype(jnp.bfloat16)
    score_of = scores.reshape(total_slots)[slot_of].reshape(token_count, TOP)
    inner_grad = group_gate[:, None] * score_of
    group_grad = jnp.sum(inner_gate * score_of, axis=1)
    return token_grad, group_grad, inner_grad, gate_grad, upper_grad, down_grad
```

```python
import functools

import jax
import jax.numpy as jnp
from jax import lax
from jax.experimental import pallas as pl
from jax.experimental.pallas import tpu as pltpu
from jax.sharding import PartitionSpec as P

LANES = 128
BF16 = jnp.bfloat16
F32 = jnp.float32


def peer_of(me, d, n):
    if n & (n - 1):
        return lax.rem(2 * n + d - me, n)
    out, bit = me, 1
    while bit < n:
        if d & bit:
            out = out + bit * (1 - 2 * lax.rem(me // bit, 2))
        bit *= 2
    return out


def barrier(partners):
    sem = pltpu.get_barrier_semaphore()
    for ep, tp in partners:
        pl.semaphore_signal(
            sem, inc=1, device_id=(ep, tp), device_id_type=pl.DeviceIdType.MESH
        )
    pl.semaphore_wait(sem, len(partners))


def remote(src, dst, send, recv, ep, tp):
    return pltpu.make_async_remote_copy(
        src_ref=src,
        dst_ref=dst,
        send_sem=send,
        recv_sem=recv,
        device_id=(ep, tp),
        device_id_type=pl.DeviceIdType.MESH,
    )


def dispatch_kernel(n_ep, n_tp, xs, gs, cs, x_out, g_out, c_out, send, recv, c_send, c_recv, stage, local):
    ep, tp = lax.axis_index("ep"), lax.axis_index("tp")
    core = lax.rem(tp, 2)
    z = tp // 2
    sibling = tp + 1 - 2 * core
    odd = lax.rem(z, 2)
    across = tp + 2 - 4 * odd
    half = xs.shape[2] // 2
    blocks = half // LANES
    lone = blocks * 3 // 8 * LANES
    both = half - 2 * lone
    base = core * half
    peers = [peer_of(ep, d, n_ep) for d in range(1, n_ep)]
    barrier([(p, tp) for p in peers] + [(ep, sibling), (ep, across)])

    def cols(start, width):
        return pl.ds(pl.multiple_of(start, LANES), width)

    mine = cols(base + odd * (lone + both), lone)
    theirs = cols(base + (1 - odd) * (lone + both), lone)
    shared = cols(base + lone, both)

    pairs = ((xs, x_out), (gs, g_out))
    started, direct = [], {}
    for d, p in enumerate(peers):
        copy = remote(cs.at[p], c_out.at[ep], c_send.at[d], c_recv.at[d], p, tp)
        copy.start()
        started.append(copy)
    for a, (src, dst) in enumerate(pairs):
        for kind, part in ((0, mine), (1, shared)):
            for d, p in enumerate(peers):
                copy = remote(
                    src.at[p, :, part], dst.at[ep, :, part],
                    send.at[a, d, kind], recv.at[a, d, kind], p, tp,
                )
                copy.start()
                direct[a, kind, d] = copy
    loads = []
    for a, (src, dst) in enumerate(pairs):
        load = pltpu.make_async_copy(src.at[ep], stage.at[a], local.at[a])
        load.start()
        loads.append(load)
    load = pltpu.make_async_copy(cs.at[ep], stage_c(c_out, ep), local.at[4])
    load.start()
    stores = [load]
    for a, (src, dst) in enumerate(pairs):
        loads[a].wait()
        store = pltpu.make_async_copy(stage.at[a], dst.at[ep], local.at[2 + a])
        store.start()
        stores.append(store)

    forwards = []
    for a, (src, dst) in enumerate(pairs):
        for kind, part in ((0, mine), (1, shared)):
            for d, p in enumerate(peers):
                direct[a, kind, d].wait_recv()
                if kind == 0:
                    copy = remote(
                        dst.at[p, :, part], dst.at[p, :, part],
                        send.at[a, d, 2], recv.at[a, d, 2], ep, across,
                    )
                    copy.start()
                    forwards.append(copy)
                    direct[a, 2, d] = remote(
                        dst.at[p, :, theirs], dst.at[p, :, theirs],
                        send.at[a, d, 2], recv.at[a, d, 2], ep, across,
                    )
                copy = remote(
                    dst.at[p, :, part], dst.at[p, :, part],
                    send.at[a, d, 3 + kind], recv.at[a, d, 3 + kind], ep, sibling,
                )
                copy.start()
                forwards.append(copy)
    for a, (src, dst) in enumerate(pairs):
        for d, p in enumerate(peers):
            direct[a, 2, d].wait_recv()
            copy = remote(
                dst.at[p, :, theirs], dst.at[p, :, theirs],
                send.at[a, d, 5], recv.at[a, d, 5], ep, sibling,
            )
            copy.start()
            forwards.append(copy)
    for a, (src, dst) in enumerate(pairs):
        for d, p in enumerate(peers):
            for kind, offset, width in (
                (3, odd * (lone + both), lone),
                (4, lone, both),
                (5, (1 - odd) * (lone + both), lone),
            ):
                part = cols((1 - core) * half + offset, width)
                remote(
                    dst.at[p, :, part], dst.at[p, :, part],
                    send.at[a, d, kind], recv.at[a, d, kind], ep, sibling,
                ).wait_recv()
    for copy in started:
        copy.wait()
    for key, copy in direct.items():
        if key[1] != 2:
            copy.wait_send()
    for copy in forwards:
        copy.wait_send()
    for store in stores:
        store.wait()


def stage_c(c_out, ep):
    return c_out.at[ep]


def dispatch(n_ep, n_tp, xs, gs, cs):
    any_spec = pl.BlockSpec(memory_space=pl.ANY)
    return pl.pallas_call(
        functools.partial(dispatch_kernel, n_ep, n_tp),
        out_shape=(
            jax.ShapeDtypeStruct(xs.shape, xs.dtype),
            jax.ShapeDtypeStruct(gs.shape, gs.dtype),
            jax.ShapeDtypeStruct(cs.shape, cs.dtype),
        ),
        in_specs=[any_spec] * 3,
        out_specs=(any_spec,) * 3,
        scratch_shapes=[
            pltpu.SemaphoreType.DMA((2, n_ep - 1, 6)),
            pltpu.SemaphoreType.DMA((2, n_ep - 1, 6)),
            pltpu.SemaphoreType.DMA((n_ep - 1,)),
            pltpu.SemaphoreType.DMA((n_ep - 1,)),
            pltpu.VMEM((2,) + xs.shape[1:], xs.dtype),
            pltpu.SemaphoreType.DMA((5,)),
        ],
        compiler_params=pltpu.CompilerParams(collective_id=0, has_side_effects=True),
    )(xs, gs, cs)


def return_kernel(n_ep, n_tp, gg, gu, wg, wu, pick, sc, out, sc_out,
                  first, first_in, second, second_in, third, third_in,
                  s1, r1, s2, r2, s3, r3, ss, rs, sl):
    ep, tp = lax.axis_index("ep"), lax.axis_index("tp")
    core = lax.rem(tp, 2)
    z = tp // 2
    nz = n_tp // 2
    sibling = tp + 1 - 2 * core
    width = out.shape[1]
    cap = second.shape[2]
    peers = [peer_of(ep, d, n_ep) for d in range(1, n_ep)]
    everyone = [(p, tp) for p in peers]
    everyone += [(ep, lax.rem(tp + k, n_tp)) for k in range(1, n_tp)]
    score_to = [(p, lax.rem(tp + k, n_tp)) for p in [ep] + peers for k in range(n_tp)][1:]
    barrier(score_to)

    sends = []
    for i, (p, t) in enumerate(score_to):
        copy = remote(sc.at[p], sc_out.at[ep, tp], ss.at[i], rs.at[i], p, t)
        copy.start()
        sends.append(copy)
    own_score = pltpu.make_async_copy(sc.at[ep], sc_out.at[ep, tp], sl)
    own_score.start()

    def partial(share):
        rows = pl.ds(pl.multiple_of(share * width, width), width)
        dims = (((1,), (1,)), ((), ()))
        return lax.dot_general(
            gg[...], wg[rows, :], dims, preferred_element_type=F32
        ) + lax.dot_general(gu[...], wu[rows, :], dims, preferred_element_type=F32)

    order = [lax.rem(z + dz, nz) for dz in range(nz - 1, -1, -1)]
    halves = []
    for i, zz in enumerate(order):
        first[i] = partial(2 * zz + 1 - core).astype(BF16)
        copy = remote(first.at[i], first_in.at[i], s1.at[i], r1.at[i], ep, sibling)
        copy.start()
        halves.append(copy)
    moves = {}
    for i, zz in enumerate(order):
        total = partial(2 * zz + core)
        halves[i].wait_recv()
        total = total + first_in[i].astype(F32)
        second[i] = total.astype(BF16).reshape(second.shape[1:])
        for d, p in enumerate(peers):
            copy = remote(
                second.at[i, p], second_in.at[i, ep], s2.at[i, d], r2.at[i, d], p, tp
            )
            copy.start()
            moves[i, d] = copy
    last = []
    for i, zz in enumerate(order):
        for d, p in enumerate(peers):
            moves[i, d].wait_recv()
        second_in[i, ep] = second[i, ep]
        rows = second_in[i].reshape(n_ep * cap, width)
        summed = jnp.dot(pick[...], rows, preferred_element_type=F32)
        third[i] = summed.astype(BF16)
        if i < nz - 1:
            copy = remote(
                third.at[i], third_in.at[i], s3.at[i], r3.at[i], ep, 2 * zz + core
            )
            copy.start()
            last.append(copy)
    total = third[nz - 1].astype(F32)
    for i in range(nz - 1):
        last[i].wait_recv()
        total = total + third_in[i].astype(F32)
    out[...] = total.astype(BF16)
    for copy in halves + list(moves.values()) + last:
        copy.wait_send()
    for copy in sends:
        copy.wait()
    own_score.wait()


def give_back(n_ep, n_tp, gg, gu, wg, wu, pick, sc):
    vmem = pl.BlockSpec(memory_space=pltpu.VMEM)
    any_spec = pl.BlockSpec(memory_space=pl.ANY)
    rows, nz = gg.shape[0], n_tp // 2
    width = wg.shape[0] // n_tp
    tokens = pick.shape[0]
    cap = rows // n_ep
    dma = pltpu.SemaphoreType.DMA
    others = n_ep * n_tp - 1
    return pl.pallas_call(
        functools.partial(return_kernel, n_ep, n_tp),
        out_shape=(
            jax.ShapeDtypeStruct((tokens, width), BF16),
            jax.ShapeDtypeStruct((n_ep, n_tp) + sc.shape[1:], F32),
        ),
        in_specs=[vmem] * 5 + [any_spec],
        out_specs=(vmem, any_spec),
        scratch_shapes=[
            pltpu.VMEM((nz, rows, width), BF16),
            pltpu.VMEM((nz, rows, width), BF16),
            pltpu.VMEM((nz, n_ep, cap, width), BF16),
            pltpu.VMEM((nz, n_ep, cap, width), BF16),
            pltpu.VMEM((nz, tokens, width), BF16),
            pltpu.VMEM((nz, tokens, width), BF16),
            dma((nz,)), dma((nz,)),
            dma((nz, n_ep - 1)), dma((nz, n_ep - 1)),
            dma((nz,)), dma((nz,)),
            dma((others,)), dma((others,)),
            dma,
        ],
        compiler_params=pltpu.CompilerParams(
            collective_id=1, has_side_effects=True, vmem_limit_bytes=56 * 1024 * 1024
        ),
    )(gg, gu, wg, wu, pick, sc)


def per_device(tokens, cotangent, routing, group_gate, inner_gate, w_gate, w_up, w_down):
    n_ep, n_tp = lax.axis_size("ep"), lax.axis_size("tp")
    tok_rows, model_width = tokens.shape
    top_k = routing.shape[1]
    cap = tok_rows * top_k * 5 // (4 * n_ep)
    rows = n_ep * cap
    experts = jnp.arange(n_ep, dtype=jnp.int32)
    route_t = routing.T
    names = jnp.sum((route_t[:, None, :] == experts[None, :, None]).astype(F32), axis=0)
    place = jnp.arange(tok_rows)
    before = (place[:, None] < place[None, :]).astype(BF16)
    rank = jnp.dot(names.astype(BF16), before, preferred_element_type=F32).astype(jnp.int32)
    slot_t = jnp.sum(
        jnp.where(
            route_t[:, None, :] == experts[None, :, None],
            experts[None, :, None] * cap + rank[None],
            0,
        ),
        axis=1,
    )
    slots = jnp.arange(rows, dtype=jnp.int32)
    hits = slots[:, None, None] == slot_t[None]
    put = jnp.any(hits, axis=1).astype(BF16)
    combine = (group_gate[:, None] * inner_gate).T
    weight = jnp.sum(jnp.where(hits, combine[None], 0.0), axis=(1, 2))
    pad = -cap % LANES
    send_weight = jnp.pad(weight.reshape(n_ep, 1, cap), ((0, 0), (0, 0), (0, pad)))

    def placed(source):
        return jnp.dot(put, source, preferred_element_type=F32).astype(BF16).reshape(
            n_ep, cap, model_width
        )

    rows_in, cot_rows, weight_in = dispatch(
        n_ep, n_tp, placed(tokens), placed(cotangent), send_weight
    )
    rows_in = rows_in.reshape(rows, model_width)
    cot_rows = cot_rows.reshape(rows, model_width)
    row_weight = weight_in[:, 0, :cap].reshape(rows)

    gate_weight, up_weight, down_weight = w_gate[0], w_up[0], w_down[0]
    gate_pre = jnp.dot(rows_in, gate_weight, preferred_element_type=F32)
    up_pre = jnp.dot(rows_in, up_weight, preferred_element_type=F32)
    sigmoid_gate = jax.nn.sigmoid(gate_pre)
    silu_gate = gate_pre * sigmoid_gate
    hidden = (silu_gate * up_pre).astype(BF16)
    scaled_cot = (row_weight[:, None] * cot_rows).astype(BF16)
    down_grad = lax.dot_general(
        hidden, scaled_cot, (((0,), (0,)), ((), ())), preferred_element_type=F32
    )
    grad_hidden = lax.dot_general(
        cot_rows, down_weight, (((1,), (1,)), ((), ())), preferred_element_type=F32
    )
    partial_scores = jnp.sum(grad_hidden * hidden.astype(F32), axis=1)
    weighted = row_weight[:, None] * grad_hidden
    grad_gate_in = (
        weighted * up_pre * sigmoid_gate * (1.0 + gate_pre * (1.0 - sigmoid_gate))
    ).astype(BF16)
    grad_up_in = (weighted * silu_gate).astype(BF16)
    gate_grad = lax.dot_general(
        rows_in, grad_gate_in, (((0,), (0,)), ((), ())), preferred_element_type=F32
    )
    upper_grad = lax.dot_general(
        rows_in, grad_up_in, (((0,), (0,)), ((), ())), preferred_element_type=F32
    )
    send_score = jnp.pad(
        partial_scores.reshape(n_ep, 1, cap), ((0, 0), (0, 0), (0, pad))
    )
    token_grad, all_scores = give_back(
        n_ep, n_tp, grad_gate_in, grad_up_in, gate_weight, up_weight, put.T, send_score
    )
    scores = jnp.sum(all_scores[:, :, 0, :cap], axis=1).reshape(rows)
    score_t = jnp.sum(jnp.where(hits, scores[:, None, None], 0.0), axis=0)
    score_of = score_t.T
    inner_grad = group_gate[:, None] * score_of
    group_grad = jnp.sum(inner_gate * score_of, axis=1)
    return (
        token_grad,
        group_grad,
        inner_grad,
        gate_grad.astype(BF16)[None],
        upper_grad.astype(BF16)[None],
        down_grad.astype(BF16)[None],
    )


def solution(mesh):
    return jax.shard_map(
        per_device,
        mesh=mesh,
        in_specs=(
            P("ep", None),
            P("ep", None),
            P("ep", None),
            P("ep"),
            P("ep", None),
            P("ep", None, "tp"),
            P("ep", None, "tp"),
            P("ep", "tp", None),
        ),
        out_specs=(
            P("ep", "tp"),
            P("ep"),
            P("ep", None),
            P("ep", None, "tp"),
            P("ep", None, "tp"),
            P("ep", "tp", None),
        ),
        check_vma=False,
    )
```

```python
import functools

import jax
import jax.numpy as jnp
from jax import lax
from jax.experimental import pallas as pl
from jax.experimental.pallas import tpu as pltpu
from jax.sharding import PartitionSpec as P

LANES = 128
BF16 = jnp.bfloat16
F32 = jnp.float32


def peer_of(me, d, n):
    if n & (n - 1):
        return lax.rem(2 * n + d - me, n)
    out, bit = me, 1
    while bit < n:
        if d & bit:
            out = out + bit * (1 - 2 * lax.rem(me // bit, 2))
        bit *= 2
    return out


def barrier(partners):
    sem = pltpu.get_barrier_semaphore()
    for ep, tp in partners:
        pl.semaphore_signal(
            sem, inc=1, device_id=(ep, tp), device_id_type=pl.DeviceIdType.MESH
        )
    pl.semaphore_wait(sem, len(partners))


def remote(src, dst, send, recv, ep, tp):
    return pltpu.make_async_remote_copy(
        src_ref=src,
        dst_ref=dst,
        send_sem=send,
        recv_sem=recv,
        device_id=(ep, tp),
        device_id_type=pl.DeviceIdType.MESH,
    )


def dispatch_kernel(n_ep, n_tp, xs, gs, cs, x_out, g_out, c_out, send, recv, c_send, c_recv, stage, local):
    ep, tp = lax.axis_index("ep"), lax.axis_index("tp")
    core = lax.rem(tp, 2)
    z = tp // 2
    sibling = tp + 1 - 2 * core
    odd = lax.rem(z, 2)
    across = tp + 2 - 4 * odd
    half = xs.shape[2] // 2
    blocks = half // LANES
    lone = blocks * 3 // 8 * LANES
    both = half - 2 * lone
    base = core * half
    peers = [peer_of(ep, d, n_ep) for d in range(1, n_ep)]
    barrier([(p, tp) for p in peers] + [(ep, sibling), (ep, across)])

    def cols(start, width):
        return pl.ds(pl.multiple_of(start, LANES), width)

    mine = cols(base + odd * (lone + both), lone)
    theirs = cols(base + (1 - odd) * (lone + both), lone)
    shared = cols(base + lone, both)

    pairs = ((xs, x_out), (gs, g_out))
    started, direct = [], {}
    for d, p in enumerate(peers):
        copy = remote(cs.at[p], c_out.at[ep], c_send.at[d], c_recv.at[d], p, tp)
        copy.start()
        started.append(copy)
    for kind, part in ((0, mine), (1, shared)):
        for a, (src, dst) in enumerate(pairs):
            for d, p in enumerate(peers):
                copy = remote(
                    src.at[p, :, part], dst.at[ep, :, part],
                    send.at[a, d, kind], recv.at[a, d, kind], p, tp,
                )
                copy.start()
                direct[a, kind, d] = copy
    loads = []
    for a, (src, dst) in enumerate(pairs):
        load = pltpu.make_async_copy(src.at[ep], stage.at[a], local.at[a])
        load.start()
        loads.append(load)
    load = pltpu.make_async_copy(cs.at[ep], stage_c(c_out, ep), local.at[4])
    load.start()
    stores = [load]
    for a, (src, dst) in enumerate(pairs):
        loads[a].wait()
        store = pltpu.make_async_copy(stage.at[a], dst.at[ep], local.at[2 + a])
        store.start()
        stores.append(store)

    forwards = []
    for kind, part in ((0, mine), (1, shared)):
        for a, (src, dst) in enumerate(pairs):
            for d, p in enumerate(peers):
                direct[a, kind, d].wait_recv()
                if kind == 0:
                    copy = remote(
                        dst.at[p, :, part], dst.at[p, :, part],
                        send.at[a, d, 2], recv.at[a, d, 2], ep, across,
                    )
                    copy.start()
                    forwards.append(copy)
                    direct[a, 2, d] = remote(
                        dst.at[p, :, theirs], dst.at[p, :, theirs],
                        send.at[a, d, 2], recv.at[a, d, 2], ep, across,
                    )
                copy = remote(
                    dst.at[p, :, part], dst.at[p, :, part],
                    send.at[a, d, 3 + kind], recv.at[a, d, 3 + kind], ep, sibling,
                )
                copy.start()
                forwards.append(copy)
    for a, (src, dst) in enumerate(pairs):
        for d, p in enumerate(peers):
            direct[a, 2, d].wait_recv()
            copy = remote(
                dst.at[p, :, theirs], dst.at[p, :, theirs],
                send.at[a, d, 5], recv.at[a, d, 5], ep, sibling,
            )
            copy.start()
            forwards.append(copy)
    for a, (src, dst) in enumerate(pairs):
        for d, p in enumerate(peers):
            for kind, offset, width in (
                (3, odd * (lone + both), lone),
                (4, lone, both),
                (5, (1 - odd) * (lone + both), lone),
            ):
                part = cols((1 - core) * half + offset, width)
                remote(
                    dst.at[p, :, part], dst.at[p, :, part],
                    send.at[a, d, kind], recv.at[a, d, kind], ep, sibling,
                ).wait_recv()
    for copy in started:
        copy.wait()
    for key, copy in direct.items():
        if key[1] != 2:
            copy.wait_send()
    for copy in forwards:
        copy.wait_send()
    for store in stores:
        store.wait()


def stage_c(c_out, ep):
    return c_out.at[ep]


def dispatch(n_ep, n_tp, xs, gs, cs):
    any_spec = pl.BlockSpec(memory_space=pl.ANY)
    return pl.pallas_call(
        functools.partial(dispatch_kernel, n_ep, n_tp),
        out_shape=(
            jax.ShapeDtypeStruct(xs.shape, xs.dtype),
            jax.ShapeDtypeStruct(gs.shape, gs.dtype),
            jax.ShapeDtypeStruct(cs.shape, cs.dtype),
        ),
        in_specs=[any_spec] * 3,
        out_specs=(any_spec,) * 3,
        scratch_shapes=[
            pltpu.SemaphoreType.DMA((2, n_ep - 1, 6)),
            pltpu.SemaphoreType.DMA((2, n_ep - 1, 6)),
            pltpu.SemaphoreType.DMA((n_ep - 1,)),
            pltpu.SemaphoreType.DMA((n_ep - 1,)),
            pltpu.VMEM((2,) + xs.shape[1:], xs.dtype),
            pltpu.SemaphoreType.DMA((5,)),
        ],
        compiler_params=pltpu.CompilerParams(collective_id=0, has_side_effects=True),
    )(xs, gs, cs)


def return_kernel(n_ep, n_tp, ggu, wg, wu, pick, hid, weight, sc, x_hbm, g_hbm,
                  out, sc_out, gate_out, up_out, down_out,
                  first, first_in, second, second_in, third, third_in,
                  xv, gv, gate_v, up_v, down_v,
                  s1, r1, s2, r2, s3, r3, ss, rs, sl, fetch, flush):
    ep, tp = lax.axis_index("ep"), lax.axis_index("tp")
    core = lax.rem(tp, 2)
    z = tp // 2
    nz = n_tp // 2
    sibling = tp + 1 - 2 * core
    width = out.shape[1]
    units = wg.shape[1]
    cap = second.shape[2]
    peers = [peer_of(ep, d, n_ep) for d in range(1, n_ep)]
    everyone = [(p, tp) for p in peers]
    everyone += [(ep, lax.rem(tp + k, n_tp)) for k in range(1, n_tp)]
    score_to = [(p, lax.rem(tp + k, n_tp)) for p in [ep] + peers for k in range(n_tp)][1:]
    fetches = [
        pltpu.make_async_copy(x_hbm, xv, fetch.at[0]),
        pltpu.make_async_copy(g_hbm, gv, fetch.at[1]),
    ]
    for copy in fetches:
        copy.start()
    barrier(score_to)

    sends = []
    for i, (p, t) in enumerate(score_to):
        copy = remote(sc.at[p], sc_out.at[ep, tp], ss.at[i], rs.at[i], p, t)
        copy.start()
        sends.append(copy)
    own_score = pltpu.make_async_copy(sc.at[ep], sc_out.at[ep, tp], sl)
    own_score.start()

    def partial(share):
        rows = pl.ds(pl.multiple_of(share * width, width), width)
        dims = (((1,), (1,)), ((), ()))
        return lax.dot_general(
            ggu[:, :units], wg[rows, :], dims, preferred_element_type=F32
        ) + lax.dot_general(ggu[:, units:], wu[rows, :], dims, preferred_element_type=F32)

    def tile(t):
        return pl.ds(pl.multiple_of(t * width, width), width)

    def gate_up_tiles(lo, hi):
        def step(t, carry):
            both = lax.dot_general(
                xv[:, tile(t)], ggu[...], (((0,), (0,)), ((), ())), preferred_element_type=F32
            ).astype(BF16)
            gate_v[tile(t), :] = both[:, :units]
            up_v[tile(t), :] = both[:, units:]
            return carry

        lax.fori_loop(lo, hi, step, 0)

    def early():
        fetches[0].wait()
        gate_up_tiles(0, n_tp // 2)

    def middle():
        gate_up_tiles(n_tp // 2, n_tp)
        for k, (src, dst) in enumerate(((gate_v, gate_out), (up_v, up_out))):
            copy = pltpu.make_async_copy(src, dst, flush.at[k])
            copy.start()
            flushes.append(copy)

    def late():
        fetches[1].wait()
        hidden_t = hid[...].T

        def step(t, carry):
            scaled = (weight[...] * gv[:, tile(t)].astype(F32)).astype(BF16)
            down_v[:, tile(t)] = jnp.dot(
                hidden_t, scaled, preferred_element_type=F32
            ).astype(BF16)
            return carry

        lax.fori_loop(0, n_tp, step, 0)
        copy = pltpu.make_async_copy(down_v, down_out, flush.at[2])
        copy.start()
        flushes.append(copy)

    flushes = []
    work = [early, middle, late]
    order = [lax.rem(z + dz, nz) for dz in range(nz - 1, -1, -1)]
    halves = []
    for i, zz in enumerate(order):
        first[i] = partial(2 * zz + 1 - core).astype(BF16)
        copy = remote(first.at[i], first_in.at[i], s1.at[i], r1.at[i], ep, sibling)
        copy.start()
        halves.append(copy)
    moves = {}
    for i, zz in enumerate(order):
        total = partial(2 * zz + core)
        halves[i].wait_recv()
        total = total + first_in[i].astype(F32)
        second[i] = total.astype(BF16).reshape(second.shape[1:])
        for d, p in enumerate(peers):
            copy = remote(
                second.at[i, p], second_in.at[i, ep], s2.at[i, d], r2.at[i, d], p, tp
            )
            copy.start()
            moves[i, d] = copy
    last = []
    for i, zz in enumerate(order):
        for job in work[i:] if i == nz - 1 else work[i : i + 1]:
            job()
        for d, p in enumerate(peers):
            moves[i, d].wait_recv()
        second_in[i, ep] = second[i, ep]
        rows = second_in[i].reshape(n_ep * cap, width)
        summed = jnp.dot(pick[...], rows, preferred_element_type=F32)
        third[i] = summed.astype(BF16)
        if i < nz - 1:
            copy = remote(
                third.at[i], third_in.at[i], s3.at[i], r3.at[i], ep, 2 * zz + core
            )
            copy.start()
            last.append(copy)
    total = third[nz - 1].astype(F32)
    for i in range(nz - 1):
        last[i].wait_recv()
        total = total + third_in[i].astype(F32)
    out[...] = total.astype(BF16)
    for copy in halves + list(moves.values()) + last:
        copy.wait_send()
    for copy in sends:
        copy.wait()
    own_score.wait()
    for copy in flushes:
        copy.wait()


def give_back(n_ep, n_tp, ggu, wg, wu, pick, hid, weight, sc, rows_in, cot_rows):
    vmem = pl.BlockSpec(memory_space=pltpu.VMEM)
    any_spec = pl.BlockSpec(memory_space=pl.ANY)
    rows, nz = ggu.shape[0], n_tp // 2
    width = wg.shape[0] // n_tp
    tokens = pick.shape[0]
    cap = rows // n_ep
    dma = pltpu.SemaphoreType.DMA
    others = n_ep * n_tp - 1
    return pl.pallas_call(
        functools.partial(return_kernel, n_ep, n_tp),
        out_shape=(
            jax.ShapeDtypeStruct((tokens, width), BF16),
            jax.ShapeDtypeStruct((n_ep, n_tp) + sc.shape[1:], F32),
            jax.ShapeDtypeStruct(wg.shape, BF16),
            jax.ShapeDtypeStruct(wu.shape, BF16),
            jax.ShapeDtypeStruct(wg.shape[::-1], BF16),
        ),
        in_specs=[vmem] * 6 + [any_spec] * 3,
        out_specs=(vmem,) + (any_spec,) * 4,
        scratch_shapes=[
            pltpu.VMEM((nz, rows, width), BF16),
            pltpu.VMEM((nz, rows, width), BF16),
            pltpu.VMEM((nz, n_ep, cap, width), BF16),
            pltpu.VMEM((nz, n_ep, cap, width), BF16),
            pltpu.VMEM((nz, tokens, width), BF16),
            pltpu.VMEM((nz, tokens, width), BF16),
            pltpu.VMEM(rows_in.shape, BF16),
            pltpu.VMEM(cot_rows.shape, BF16),
            pltpu.VMEM(wg.shape, BF16),
            pltpu.VMEM(wu.shape, BF16),
            pltpu.VMEM(wg.shape[::-1], BF16),
            dma((nz,)), dma((nz,)),
            dma((nz, n_ep - 1)), dma((nz, n_ep - 1)),
            dma((nz,)), dma((nz,)),
            dma((others,)), dma((others,)),
            dma,
            dma((2,)),
            dma((3,)),
        ],
        compiler_params=pltpu.CompilerParams(
            collective_id=1, has_side_effects=True, vmem_limit_bytes=56 * 1024 * 1024
        ),
    )(ggu, wg, wu, pick, hid, weight, sc, rows_in, cot_rows)


def per_device(tokens, cotangent, routing, group_gate, inner_gate, w_gate, w_up, w_down):
    n_ep, n_tp = lax.axis_size("ep"), lax.axis_size("tp")
    tok_rows, model_width = tokens.shape
    top_k = routing.shape[1]
    cap = tok_rows * top_k * 5 // (4 * n_ep)
    rows = n_ep * cap
    experts = jnp.arange(n_ep, dtype=jnp.int32)
    route_t = routing.T
    names = jnp.sum((route_t[:, None, :] == experts[None, :, None]).astype(F32), axis=0)
    place = jnp.arange(tok_rows)
    before = (place[:, None] < place[None, :]).astype(BF16)
    rank = jnp.dot(names.astype(BF16), before, preferred_element_type=F32).astype(jnp.int32)
    slot_t = jnp.sum(
        jnp.where(
            route_t[:, None, :] == experts[None, :, None],
            experts[None, :, None] * cap + rank[None],
            0,
        ),
        axis=1,
    )
    slots = jnp.arange(rows, dtype=jnp.int32)
    hits = slots[:, None, None] == slot_t[None]
    put = jnp.any(hits, axis=1).astype(BF16)
    combine = (group_gate[:, None] * inner_gate).T
    weight = jnp.sum(jnp.where(hits, combine[None], 0.0), axis=(1, 2))
    pad = -cap % LANES
    send_weight = jnp.pad(weight.reshape(n_ep, 1, cap), ((0, 0), (0, 0), (0, pad)))

    def placed(source):
        return jnp.dot(put, source, preferred_element_type=F32).astype(BF16).reshape(
            n_ep, cap, model_width
        )

    rows_in, cot_rows, weight_in = dispatch(
        n_ep, n_tp, placed(tokens), placed(cotangent), send_weight
    )
    rows_in = rows_in.reshape(rows, model_width)
    cot_rows = cot_rows.reshape(rows, model_width)
    row_weight = weight_in[:, 0, :cap].reshape(rows)

    gate_weight, up_weight, down_weight = w_gate[0], w_up[0], w_down[0]
    gate_pre = jnp.dot(rows_in, gate_weight, preferred_element_type=F32)
    up_pre = jnp.dot(rows_in, up_weight, preferred_element_type=F32)
    sigmoid_gate = jax.nn.sigmoid(gate_pre)
    silu_gate = gate_pre * sigmoid_gate
    hidden = (silu_gate * up_pre).astype(BF16)
    grad_hidden = lax.dot_general(
        cot_rows, down_weight, (((1,), (1,)), ((), ())), preferred_element_type=F32
    )
    partial_scores = jnp.sum(grad_hidden * hidden.astype(F32), axis=1)
    weighted = row_weight[:, None] * grad_hidden
    grad_gate_in = (
        weighted * up_pre * sigmoid_gate * (1.0 + gate_pre * (1.0 - sigmoid_gate))
    ).astype(BF16)
    grad_up_in = (weighted * silu_gate).astype(BF16)
    send_score = jnp.pad(
        partial_scores.reshape(n_ep, 1, cap), ((0, 0), (0, 0), (0, pad))
    )
    token_grad, all_scores, gate_grad, upper_grad, down_grad = give_back(
        n_ep, n_tp, jnp.concatenate([grad_gate_in, grad_up_in], axis=1),
        gate_weight, up_weight, put.T, hidden, row_weight[:, None], send_score,
        rows_in, cot_rows,
    )
    scores = jnp.sum(all_scores[:, :, 0, :cap], axis=1).reshape(rows)
    score_t = jnp.sum(jnp.where(hits, scores[:, None, None], 0.0), axis=0)
    score_of = score_t.T
    inner_grad = group_gate[:, None] * score_of
    group_grad = jnp.sum(inner_gate * score_of, axis=1)
    return (
        token_grad,
        group_grad,
        inner_grad,
        gate_grad[None],
        upper_grad[None],
        down_grad[None],
    )


def solution(mesh):
    return jax.shard_map(
        per_device,
        mesh=mesh,
        in_specs=(
            P("ep", None),
            P("ep", None),
            P("ep", None),
            P("ep"),
            P("ep", None),
            P("ep", None, "tp"),
            P("ep", None, "tp"),
            P("ep", "tp", None),
        ),
        out_specs=(
            P("ep", "tp"),
            P("ep"),
            P("ep", None),
            P("ep", None, "tp"),
            P("ep", None, "tp"),
            P("ep", "tp", None),
        ),
        check_vma=False,
    )
```

```python
import functools

import jax
import jax.numpy as jnp
from jax import lax
from jax.experimental import pallas as pl
from jax.experimental.pallas import tpu as pltpu
from jax.sharding import PartitionSpec as P

LANES = 128
BF16 = jnp.bfloat16
F32 = jnp.float32


def peer_of(me, d, n):
    if n & (n - 1):
        return lax.rem(2 * n + d - me, n)
    out, bit = me, 1
    while bit < n:
        if d & bit:
            out = out + bit * (1 - 2 * lax.rem(me // bit, 2))
        bit *= 2
    return out


def greet(partners):
    sem = pltpu.get_barrier_semaphore()
    for ep, tp in partners:
        pl.semaphore_signal(
            sem, inc=1, device_id=(ep, tp), device_id_type=pl.DeviceIdType.MESH
        )
    return lambda: pl.semaphore_wait(sem, len(partners))


def remote(src, dst, send, recv, ep, tp):
    return pltpu.make_async_remote_copy(
        src_ref=src,
        dst_ref=dst,
        send_sem=send,
        recv_sem=recv,
        device_id=(ep, tp),
        device_id_type=pl.DeviceIdType.MESH,
    )


def dispatch_kernel(n_ep, n_tp, xs, gs, cs, x_out, g_out, c_out, send, recv, c_send, c_recv, stage, local):
    ep, tp = lax.axis_index("ep"), lax.axis_index("tp")
    core = lax.rem(tp, 2)
    z = tp // 2
    sibling = tp + 1 - 2 * core
    odd = lax.rem(z, 2)
    across = tp + 2 - 4 * odd
    half = xs.shape[2] // 2
    blocks = half // LANES
    lone = blocks * 3 // 8 * LANES
    both = half - 2 * lone
    base = core * half
    peers = [peer_of(ep, d, n_ep) for d in range(1, n_ep)]
    greet([(p, tp) for p in peers] + [(ep, sibling), (ep, across)])()

    def cols(start, width):
        return pl.ds(pl.multiple_of(start, LANES), width)

    mine = cols(base + odd * (lone + both), lone)
    theirs = cols(base + (1 - odd) * (lone + both), lone)
    shared = cols(base + lone, both)

    pairs = ((xs, x_out), (gs, g_out))
    started, direct = [], {}
    for d, p in enumerate(peers):
        copy = remote(cs.at[p], c_out.at[ep], c_send.at[d], c_recv.at[d], p, tp)
        copy.start()
        started.append(copy)
    for kind, part in ((0, mine), (1, shared)):
        for a, (src, dst) in enumerate(pairs):
            for d, p in enumerate(peers):
                copy = remote(
                    src.at[p, :, part], dst.at[ep, :, part],
                    send.at[a, d, kind], recv.at[a, d, kind], p, tp,
                )
                copy.start()
                direct[a, kind, d] = copy
    loads = []
    for a, (src, dst) in enumerate(pairs):
        load = pltpu.make_async_copy(src.at[ep], stage.at[a], local.at[a])
        load.start()
        loads.append(load)
    load = pltpu.make_async_copy(cs.at[ep], stage_c(c_out, ep), local.at[4])
    load.start()
    stores = [load]
    for a, (src, dst) in enumerate(pairs):
        loads[a].wait()
        store = pltpu.make_async_copy(stage.at[a], dst.at[ep], local.at[2 + a])
        store.start()
        stores.append(store)

    forwards = []
    for kind, part in ((0, mine), (1, shared)):
        for a, (src, dst) in enumerate(pairs):
            for d, p in enumerate(peers):
                direct[a, kind, d].wait_recv()
                if kind == 0:
                    copy = remote(
                        dst.at[p, :, part], dst.at[p, :, part],
                        send.at[a, d, 2], recv.at[a, d, 2], ep, across,
                    )
                    copy.start()
                    forwards.append(copy)
                    direct[a, 2, d] = remote(
                        dst.at[p, :, theirs], dst.at[p, :, theirs],
                        send.at[a, d, 2], recv.at[a, d, 2], ep, across,
                    )
                copy = remote(
                    dst.at[p, :, part], dst.at[p, :, part],
                    send.at[a, d, 3 + kind], recv.at[a, d, 3 + kind], ep, sibling,
                )
                copy.start()
                forwards.append(copy)
    for a, (src, dst) in enumerate(pairs):
        for d, p in enumerate(peers):
            direct[a, 2, d].wait_recv()
            copy = remote(
                dst.at[p, :, theirs], dst.at[p, :, theirs],
                send.at[a, d, 5], recv.at[a, d, 5], ep, sibling,
            )
            copy.start()
            forwards.append(copy)
    for a, (src, dst) in enumerate(pairs):
        for d, p in enumerate(peers):
            for kind, offset, width in (
                (3, odd * (lone + both), lone),
                (4, lone, both),
                (5, (1 - odd) * (lone + both), lone),
            ):
                part = cols((1 - core) * half + offset, width)
                remote(
                    dst.at[p, :, part], dst.at[p, :, part],
                    send.at[a, d, kind], recv.at[a, d, kind], ep, sibling,
                ).wait_recv()
    for copy in started:
        copy.wait()
    for key, copy in direct.items():
        if key[1] != 2:
            copy.wait_send()
    for copy in forwards:
        copy.wait_send()
    for store in stores:
        store.wait()


def stage_c(c_out, ep):
    return c_out.at[ep]


def dispatch(n_ep, n_tp, xs, gs, cs):
    any_spec = pl.BlockSpec(memory_space=pl.ANY)
    return pl.pallas_call(
        functools.partial(dispatch_kernel, n_ep, n_tp),
        out_shape=(
            jax.ShapeDtypeStruct(xs.shape, xs.dtype),
            jax.ShapeDtypeStruct(gs.shape, gs.dtype),
            jax.ShapeDtypeStruct(cs.shape, cs.dtype),
        ),
        in_specs=[any_spec] * 3,
        out_specs=(any_spec,) * 3,
        scratch_shapes=[
            pltpu.SemaphoreType.DMA((2, n_ep - 1, 6)),
            pltpu.SemaphoreType.DMA((2, n_ep - 1, 6)),
            pltpu.SemaphoreType.DMA((n_ep - 1,)),
            pltpu.SemaphoreType.DMA((n_ep - 1,)),
            pltpu.VMEM((2,) + xs.shape[1:], xs.dtype),
            pltpu.SemaphoreType.DMA((5,)),
        ],
        compiler_params=pltpu.CompilerParams(collective_id=0, has_side_effects=True),
    )(xs, gs, cs)


def return_kernel(n_ep, n_tp, ggu, pick, hid, weight, sc, x_hbm, g_hbm, wg_hbm, wu_hbm,
                  out, sc_out, gate_out, up_out, down_out,
                  first, first_in, second, second_in, third, third_in,
                  xv, gv, gate_v, up_v, down_v, wg, wu,
                  s1, r1, s2, r2, s3, r3, ss, rs, sl, fetch, flush, w_sem):
    ep, tp = lax.axis_index("ep"), lax.axis_index("tp")
    core = lax.rem(tp, 2)
    z = tp // 2
    nz = n_tp // 2
    sibling = tp + 1 - 2 * core
    width = out.shape[1]
    units = wg.shape[1]
    cap = second.shape[2]
    peers = [peer_of(ep, d, n_ep) for d in range(1, n_ep)]
    score_to = [(p, lax.rem(tp + k, n_tp)) for p in [ep] + peers for k in range(n_tp)][1:]
    order = [lax.rem(z + dz, nz) for dz in range(nz - 1, -1, -1)]
    weight_fetches = []
    for i, zz in enumerate(order):
        rows = pl.ds(pl.multiple_of(2 * zz * width, width), 2 * width)
        for k, (src, dst) in enumerate(((wg_hbm, wg), (wu_hbm, wu))):
            copy = pltpu.make_async_copy(src.at[rows], dst.at[rows], w_sem.at[k, i])
            copy.start()
            weight_fetches.append(copy)
    fetches = [
        pltpu.make_async_copy(x_hbm, xv, fetch.at[0]),
        pltpu.make_async_copy(g_hbm, gv, fetch.at[1]),
    ]
    for copy in fetches:
        copy.start()
    arrived = greet(score_to)

    def partial(share):
        rows = pl.ds(pl.multiple_of(share * width, width), width)
        dims = (((1,), (1,)), ((), ()))
        return lax.dot_general(
            ggu[:, :units], wg[rows, :], dims, preferred_element_type=F32
        ) + lax.dot_general(ggu[:, units:], wu[rows, :], dims, preferred_element_type=F32)

    def tile(t):
        return pl.ds(pl.multiple_of(t * width, width), width)

    def gate_up_tiles(lo, hi):
        def step(t, carry):
            both = lax.dot_general(
                xv[:, tile(t)], ggu[...], (((0,), (0,)), ((), ())), preferred_element_type=F32
            ).astype(BF16)
            gate_v[tile(t), :] = both[:, :units]
            up_v[tile(t), :] = both[:, units:]
            return carry

        lax.fori_loop(lo, hi, step, 0)

    def early():
        fetches[0].wait()
        gate_up_tiles(0, n_tp // 2)

    def middle():
        gate_up_tiles(n_tp // 2, n_tp)
        for k, (src, dst) in enumerate(((gate_v, gate_out), (up_v, up_out))):
            copy = pltpu.make_async_copy(src, dst, flush.at[k])
            copy.start()
            flushes.append(copy)

    def late():
        fetches[1].wait()
        hidden_t = hid[...].T

        def step(t, carry):
            scaled = (weight[...] * gv[:, tile(t)].astype(F32)).astype(BF16)
            down_v[:, tile(t)] = jnp.dot(
                hidden_t, scaled, preferred_element_type=F32
            ).astype(BF16)
            return carry

        lax.fori_loop(0, n_tp, step, 0)
        copy = pltpu.make_async_copy(down_v, down_out, flush.at[2])
        copy.start()
        flushes.append(copy)

    flushes = []
    work = [early, middle, late]
    halves = []

    def prepare(i):
        for copy in weight_fetches[2 * i : 2 * i + 2]:
            copy.wait()
        first[i] = partial(2 * order[i] + 1 - core).astype(BF16)

    def push(i):
        copy = remote(first.at[i], first_in.at[i], s1.at[i], r1.at[i], ep, sibling)
        copy.start()
        halves.append(copy)

    ahead = min(2, nz)
    for i in range(ahead):
        prepare(i)
    arrived()
    for i in range(ahead):
        push(i)
    sends = []
    for i, (p, t) in enumerate(score_to):
        copy = remote(sc.at[p], sc_out.at[ep, tp], ss.at[i], rs.at[i], p, t)
        copy.start()
        sends.append(copy)
    own_score = pltpu.make_async_copy(sc.at[ep], sc_out.at[ep, tp], sl)
    own_score.start()
    moves = {}
    for i, zz in enumerate(order):
        total = partial(2 * zz + core)
        halves[i].wait_recv()
        total = total + first_in[i].astype(F32)
        second[i] = total.astype(BF16).reshape(second.shape[1:])
        for d, p in enumerate(peers):
            copy = remote(
                second.at[i, p], second_in.at[i, ep], s2.at[i, d], r2.at[i, d], p, tp
            )
            copy.start()
            moves[i, d] = copy
        if i + ahead < nz:
            prepare(i + ahead)
            push(i + ahead)
    last = []
    for i, zz in enumerate(order):
        for job in work[i:] if i == nz - 1 else work[i : i + 1]:
            job()
        for d, p in enumerate(peers):
            moves[i, d].wait_recv()
        second_in[i, ep] = second[i, ep]
        rows = second_in[i].reshape(n_ep * cap, width)
        summed = jnp.dot(pick[...], rows, preferred_element_type=F32)
        third[i] = summed.astype(BF16)
        if i < nz - 1:
            copy = remote(
                third.at[i], third_in.at[i], s3.at[i], r3.at[i], ep, 2 * zz + core
            )
            copy.start()
            last.append(copy)
    total = third[nz - 1].astype(F32)
    for i in range(nz - 1):
        last[i].wait_recv()
        total = total + third_in[i].astype(F32)
    out[...] = total.astype(BF16)
    for copy in halves + list(moves.values()) + last:
        copy.wait_send()
    for copy in sends:
        copy.wait()
    own_score.wait()
    for copy in flushes:
        copy.wait()


def give_back(n_ep, n_tp, ggu, wg, wu, pick, hid, weight, sc, rows_in, cot_rows):
    vmem = pl.BlockSpec(memory_space=pltpu.VMEM)
    any_spec = pl.BlockSpec(memory_space=pl.ANY)
    rows, nz = ggu.shape[0], n_tp // 2
    width = wg.shape[0] // n_tp
    tokens = pick.shape[0]
    cap = rows // n_ep
    dma = pltpu.SemaphoreType.DMA
    others = n_ep * n_tp - 1
    return pl.pallas_call(
        functools.partial(return_kernel, n_ep, n_tp),
        out_shape=(
            jax.ShapeDtypeStruct((tokens, width), BF16),
            jax.ShapeDtypeStruct((n_ep, n_tp) + sc.shape[1:], F32),
            jax.ShapeDtypeStruct(wg.shape, BF16),
            jax.ShapeDtypeStruct(wu.shape, BF16),
            jax.ShapeDtypeStruct(wg.shape[::-1], BF16),
        ),
        in_specs=[vmem] * 4 + [any_spec] * 5,
        out_specs=(vmem,) + (any_spec,) * 4,
        scratch_shapes=[
            pltpu.VMEM((nz, rows, width), BF16),
            pltpu.VMEM((nz, rows, width), BF16),
            pltpu.VMEM((nz, n_ep, cap, width), BF16),
            pltpu.VMEM((nz, n_ep, cap, width), BF16),
            pltpu.VMEM((nz, tokens, width), BF16),
            pltpu.VMEM((nz, tokens, width), BF16),
            pltpu.VMEM(rows_in.shape, BF16),
            pltpu.VMEM(cot_rows.shape, BF16),
            pltpu.VMEM(wg.shape, BF16),
            pltpu.VMEM(wu.shape, BF16),
            pltpu.VMEM(wg.shape[::-1], BF16),
            pltpu.VMEM(wg.shape, BF16),
            pltpu.VMEM(wu.shape, BF16),
            dma((nz,)), dma((nz,)),
            dma((nz, n_ep - 1)), dma((nz, n_ep - 1)),
            dma((nz,)), dma((nz,)),
            dma((others,)), dma((others,)),
            dma,
            dma((2,)),
            dma((3,)),
            dma((2, nz)),
        ],
        compiler_params=pltpu.CompilerParams(
            collective_id=1, has_side_effects=True, vmem_limit_bytes=56 * 1024 * 1024
        ),
    )(ggu, pick, hid, weight, sc, rows_in, cot_rows, wg, wu)


def per_device(tokens, cotangent, routing, group_gate, inner_gate, w_gate, w_up, w_down):
    n_ep, n_tp = lax.axis_size("ep"), lax.axis_size("tp")
    tok_rows, model_width = tokens.shape
    top_k = routing.shape[1]
    cap = tok_rows * top_k * 5 // (4 * n_ep)
    rows = n_ep * cap
    experts = jnp.arange(n_ep, dtype=jnp.int32)
    route_t = routing.T
    names = jnp.sum((route_t[:, None, :] == experts[None, :, None]).astype(F32), axis=0)
    place = jnp.arange(tok_rows)
    before = (place[:, None] < place[None, :]).astype(BF16)
    rank = jnp.dot(names.astype(BF16), before, preferred_element_type=F32).astype(jnp.int32)
    slot_t = jnp.sum(
        jnp.where(
            route_t[:, None, :] == experts[None, :, None],
            experts[None, :, None] * cap + rank[None],
            0,
        ),
        axis=1,
    )
    slots = jnp.arange(rows, dtype=jnp.int32)
    hits = slots[:, None, None] == slot_t[None]
    put = jnp.any(hits, axis=1).astype(BF16)
    combine = (group_gate[:, None] * inner_gate).T
    weight = jnp.sum(jnp.where(hits, combine[None], 0.0), axis=(1, 2))
    pad = -cap % LANES
    send_weight = jnp.pad(weight.reshape(n_ep, 1, cap), ((0, 0), (0, 0), (0, pad)))

    def placed(source):
        return jnp.dot(put, source, preferred_element_type=F32).astype(BF16).reshape(
            n_ep, cap, model_width
        )

    rows_in, cot_rows, weight_in = dispatch(
        n_ep, n_tp, placed(tokens), placed(cotangent), send_weight
    )
    rows_in = rows_in.reshape(rows, model_width)
    cot_rows = cot_rows.reshape(rows, model_width)
    row_weight = weight_in[:, 0, :cap].reshape(rows)

    gate_weight, up_weight, down_weight = w_gate[0], w_up[0], w_down[0]
    gate_pre = jnp.dot(rows_in, gate_weight, preferred_element_type=F32)
    up_pre = jnp.dot(rows_in, up_weight, preferred_element_type=F32)
    sigmoid_gate = jax.nn.sigmoid(gate_pre)
    silu_gate = gate_pre * sigmoid_gate
    hidden = (silu_gate * up_pre).astype(BF16)
    grad_hidden = lax.dot_general(
        cot_rows, down_weight, (((1,), (1,)), ((), ())), preferred_element_type=F32
    )
    partial_scores = jnp.sum(grad_hidden * hidden.astype(F32), axis=1)
    weighted = row_weight[:, None] * grad_hidden
    grad_gate_in = (
        weighted * up_pre * sigmoid_gate * (1.0 + gate_pre * (1.0 - sigmoid_gate))
    ).astype(BF16)
    grad_up_in = (weighted * silu_gate).astype(BF16)
    send_score = jnp.pad(
        partial_scores.reshape(n_ep, 1, cap), ((0, 0), (0, 0), (0, pad))
    )
    token_grad, all_scores, gate_grad, upper_grad, down_grad = give_back(
        n_ep, n_tp, jnp.concatenate([grad_gate_in, grad_up_in], axis=1),
        gate_weight, up_weight, put.T, hidden, row_weight[:, None], send_score,
        rows_in, cot_rows,
    )
    scores = jnp.sum(all_scores[:, :, 0, :cap], axis=1).reshape(rows)
    score_t = jnp.sum(jnp.where(hits, scores[:, None, None], 0.0), axis=0)
    score_of = score_t.T
    inner_grad = group_gate[:, None] * score_of
    group_grad = jnp.sum(inner_gate * score_of, axis=1)
    return (
        token_grad,
        group_grad,
        inner_grad,
        gate_grad[None],
        upper_grad[None],
        down_grad[None],
    )


def solution(mesh):
    return jax.shard_map(
        per_device,
        mesh=mesh,
        in_specs=(
            P("ep", None),
            P("ep", None),
            P("ep", None),
            P("ep"),
            P("ep", None),
            P("ep", None, "tp"),
            P("ep", None, "tp"),
            P("ep", "tp", None),
        ),
        out_specs=(
            P("ep", "tp"),
            P("ep"),
            P("ep", None),
            P("ep", None, "tp"),
            P("ep", None, "tp"),
            P("ep", "tp", None),
        ),
        check_vma=False,
    )
```
